32 devices in a mesh: sp: 8 (over z, y), tp: 4 (over x, core).
Axes of the slice: x: 2, y: 2, z: 4, core: 2. Of those that a mesh axis runs over, the one named last changes fastest.
Arguments:
- tokens: bfloat16 [4096, 2048], P('sp', 'tp'), may hold values from -6 to 6
- norm_gain: float32 [2048], replicated, may hold values from 0.1 to 1.9
- query_weight: bfloat16 [2048, 2048], P('sp', 'tp'), may hold values from -0.125 to 0.125
- key_weight: bfloat16 [2048, 512], P('sp', 'tp'), may hold values from -0.125 to 0.125
- value_weight: bfloat16 [2048, 512], P('sp', 'tp'), may hold values from -0.125 to 0.125
- pool_in_weight: bfloat16 [2048, 1024], P('sp', 'tp'), may hold values from -0.125 to 0.125
- pool_mix_weight: bfloat16 [4, 256, 256], P('tp'), may hold values from -0.375 to 0.375
- sink_logit: float32 [32], P('tp'), may hold values from -300 to 300
- out_pool_weight: bfloat16 [1024, 2048], P('tp', 'sp'), may hold values from -0.109375 to 0.109375
- out_attn_weight: bfloat16 [2048, 2048], P('tp', 'sp'), may hold values from -1.25 to 1.25
Outputs:
- mixed: bfloat16 [4096, 2048], P('sp', 'tp')
- log_weight: float32 [32, 4096], P('tp', 'sp')
The draws below stay inside these ranges and needn't reach their ends.
All inputs are finite; a program needn't handle non-finite values.
Results may differ from the reference program's by a relative error of at most 0.012.
Values may be sent and summed in bfloat16 or wider, within the bound.
A program may use at most 64 MiB of HBM per device.

```python
import jax
import jax.numpy as jnp
from jax import lax

D = 2048
HQ = 32
KVH = 8
HD = 64
GROUPS = 4
POOL_GC = 256
WINDOW = 128
GRID_W = 64
POOL_WIDTH = 1024
TOKENS = 4096
N_TP = 4


def draw_sink_logit(key, part):
    heads_per_group = HQ // KVH
    drawn = jax.random.uniform(jax.random.fold_in(key, 11), (KVH, heads_per_group), jnp.float32, 2.0, 6.0)
    return drawn.reshape(HQ)


def block_scale(key, shape, cuts, low, largest):
    gain, own = 1.0, jax.random.fold_in(key, 6)
    for position, parts in cuts:
        heights = jnp.exp(jax.random.uniform(jax.random.fold_in(own, position), (parts,), jnp.float32, low / len(cuts), largest / len(cuts)))
        gain = gain * jnp.repeat(heights, shape[position] // parts).reshape([-1 if axis == position else 1 for axis in range(len(shape))])
    return gain


def scatter_about(stream_key, dims, spread, bound, pieces=(), kind=jnp.bfloat16):
    values = jax.random.normal(stream_key, dims, jnp.float32) * spread
    if len(pieces) > 0:
        values = block_scale(stream_key, dims, pieces, -0.22, 0.18) * values
    return jnp.clip(values, min=-bound, max=bound).astype(kind)


def setup_inputs(seed: int = 0) -> dict:
    streams_of = jax.random.split(jax.random.key(seed), 11)
    tokens = scatter_about(streams_of[0], (TOKENS, D), 1.0, 6.0, ((0, 8), (1, 4)))
    norm_gain = jnp.clip(1.0 + 0.18 * jax.random.normal(streams_of[1], (D,), jnp.float32), 0.1, 1.9)
    query_weight = scatter_about(streams_of[2], (D, HQ * HD), D ** -0.5, 0.125, ((0, 8), (1, 4)))
    key_weight = scatter_about(streams_of[3], (D, KVH * HD), D ** -0.5, 0.125, ((0, 8), (1, 4)))
    value_weight = scatter_about(streams_of[4], (D, KVH * HD), D ** -0.5, 0.125, ((0, 8), (1, 4)))
    pool_in_weight = scatter_about(streams_of[5], (D, POOL_WIDTH), D ** -0.5, 0.125, ((0, 8), (1, 4)))
    pool_mix_weight = scatter_about(streams_of[6], (GROUPS, POOL_GC, POOL_GC), POOL_GC ** -0.5, 0.375, ((0, 4),))
    sink_logit = draw_sink_logit(jax.random.fold_in(streams_of[10], 71), 0)
    out_pool_weight = scatter_about(streams_of[8], (POOL_WIDTH, D), (POOL_WIDTH + HQ * HD) ** -0.5, 0.109375, ((0, 4), (1, 8)))
    out_attn_weight = scatter_about(streams_of[9], (HQ * HD, D), ((POOL_WIDTH + HQ * HD) // 144) ** -0.5, 1.25, ((0, 4), (1, 8)))
    return {"tokens": tokens, "norm_gain": norm_gain, "query_weight": query_weight, "key_weight": key_weight, "value_weight": value_weight, "pool_in_weight": pool_in_weight, "pool_mix_weight": pool_mix_weight, "sink_logit": sink_logit, "out_pool_weight": out_pool_weight, "out_attn_weight": out_attn_weight}


norm_eps = 1e-06
rope_base = 10000.0
pool_reach = 8
neg_fill = -1e+30

def rope_tables(positions, head_dim):
    n_freq = head_dim // 4
    freqs = rope_base ** (-jnp.arange(n_freq, dtype=jnp.float32) / n_freq)
    rows = (positions // GRID_W).astype(jnp.float32)
    columns = (positions % GRID_W).astype(jnp.float32)
    row_angle = rows[:, None] * freqs[None, :]
    col_angle = columns[:, None] * freqs[None, :]
    return (jnp.cos(row_angle), jnp.sin(row_angle), jnp.cos(col_angle), jnp.sin(col_angle))

def rotate_half(values, cosine, sine):
    middle = values.shape[-1] // 2
    first = values[..., :middle]
    second = values[..., middle:]
    return jnp.concatenate([first * cosine - second * sine, second * cosine + first * sine], -1)

def rotate_heads(values, tables, head_dim):
    rows_count = values.shape[0]
    shaped = values.astype(jnp.float32).reshape(rows_count, -1, head_dim)
    cos_r, sin_r, cos_c, sin_c = [table[:, None, :] for table in tables]
    split = head_dim // 2
    turned = jnp.concatenate([rotate_half(shaped[..., :split], cos_r, sin_r), rotate_half(shaped[..., split:], cos_c, sin_c)], -1)
    return turned.reshape(rows_count, -1).astype(jnp.bfloat16)

def pool_group(extended, own, positions, half_width, seq_total):
    rows_count = own.shape[0]
    summed = jnp.zeros(own.shape, jnp.float32)
    counted = jnp.zeros((rows_count,), jnp.float32)
    for shift_by in range(-pool_reach, pool_reach):
        source = positions + shift_by
        inside = (shift_by >= -half_width) & (shift_by < half_width) & (source >= 0) & (source < seq_total)
        window_rows = extended[pool_reach + shift_by:pool_reach + shift_by + rows_count].astype(jnp.float32)
        summed = summed + jnp.where(inside[:, None], window_rows, 0.0)
        counted = counted + inside.astype(jnp.float32)
    return (summed / counted[:, None] - own.astype(jnp.float32)).astype(jnp.bfloat16)

def attend_block(queries, keys, values, sink, query_pos, key_pos, seq_total):
    scores = jnp.einsum('qhgd,khd->hgqk', queries.astype(jnp.float32), keys.astype(jnp.float32)) * HD ** (-0.5)
    valid = (jnp.abs(query_pos[:, None] - key_pos[None, :]) <= WINDOW) & (key_pos >= 0)[None, :] & (key_pos < seq_total)[None, :]
    scores = jnp.where(valid, scores, neg_fill)
    row_top = jnp.maximum(lax.optimization_barrier(jnp.max(scores, -1)), sink[:, :, None])
    exps = jnp.exp(scores - row_top[..., None])
    row_total = lax.optimization_barrier(jnp.sum(exps, -1)) + jnp.exp(sink[:, :, None] - row_top)
    weights = (exps / row_total[..., None]).astype(jnp.bfloat16)
    attended = jnp.einsum('hgqk,khd->qhgd', weights.astype(jnp.float32), values.astype(jnp.float32))
    return (attended.astype(jnp.bfloat16), row_top + jnp.log(row_total))

def reference(tokens, norm_gain, query_weight, key_weight, value_weight, pool_in_weight, pool_mix_weight, sink_logit, out_pool_weight, out_attn_weight):
    seq_total = tokens.shape[0]
    wide = tokens.astype(jnp.float32)
    normed = (wide * lax.rsqrt(lax.optimization_barrier(jnp.mean(wide * wide, -1, keepdims=True)) + norm_eps) * norm_gain).astype(jnp.bfloat16)
    query = jnp.dot(normed, query_weight, preferred_element_type=jnp.float32).astype(jnp.bfloat16)
    key = jnp.dot(normed, key_weight, preferred_element_type=jnp.float32).astype(jnp.bfloat16)
    value = jnp.dot(normed, value_weight, preferred_element_type=jnp.float32).astype(jnp.bfloat16)
    pool_input = jnp.dot(normed, pool_in_weight, preferred_element_type=jnp.float32).astype(jnp.bfloat16)
    positions = jnp.arange(seq_total, dtype=jnp.int32)
    tables = rope_tables(positions, HD)
    rot_query = rotate_heads(query, tables, HD)
    rot_key = rotate_heads(key, tables, HD)
    pool_parts = []
    for group in range(GROUPS):
        own = pool_input[:, group * POOL_GC:(group + 1) * POOL_GC]
        extended = jnp.pad(own, ((pool_reach, pool_reach), (0, 0)))
        pooled = pool_group(extended, own, positions, 2 ** group, seq_total)
        pool_parts.append(jnp.dot(pooled, pool_mix_weight[group], preferred_element_type=jnp.float32).astype(jnp.bfloat16))
    pool_out = jnp.concatenate(pool_parts, 1)
    grp = HQ // KVH
    query_heads = rot_query.reshape(seq_total, KVH, grp, HD)
    key_pad = jnp.pad(rot_key.reshape(seq_total, KVH, HD), ((WINDOW, WINDOW), (0, 0), (0, 0)))
    value_pad = jnp.pad(value.reshape(seq_total, KVH, HD), ((WINDOW, WINDOW), (0, 0), (0, 0)))
    sink = sink_logit.reshape(KVH, grp)
    block_rows = 512

    def block_fn(block_index):
        start = (block_index * block_rows).astype(jnp.int32)
        queries = lax.dynamic_slice_in_dim(query_heads, start, block_rows, 0)
        keys = lax.dynamic_slice_in_dim(key_pad, start, block_rows + 2 * WINDOW, 0)
        values = lax.dynamic_slice_in_dim(value_pad, start, block_rows + 2 * WINDOW, 0)
        query_pos = start + jnp.arange(block_rows, dtype=jnp.int32)
        key_pos = start - WINDOW + jnp.arange(block_rows + 2 * WINDOW, dtype=jnp.int32)
        return attend_block(queries, keys, values, sink, query_pos, key_pos, seq_total)
    n_blocks = seq_total // block_rows
    attended, log_blocks = lax.map(block_fn, jnp.arange(n_blocks, dtype=jnp.int32))
    attended = attended.reshape(seq_total, HQ * HD)
    log_weight = jnp.moveaxis(log_blocks.reshape(n_blocks, HQ, block_rows), 0, 1).reshape(HQ, seq_total)
    attn_group = HQ * HD // N_TP
    mixed = jnp.zeros((seq_total, D), jnp.float32)
    for part in range(N_TP):
        term = jnp.dot(pool_out[:, part * POOL_GC:(part + 1) * POOL_GC], out_pool_weight[part * POOL_GC:(part + 1) * POOL_GC], preferred_element_type=jnp.float32)
        term = term + jnp.dot(attended[:, part * attn_group:(part + 1) * attn_group], out_attn_weight[part * attn_group:(part + 1) * attn_group], preferred_element_type=jnp.float32)
        rounded = lax.optimization_barrier(term.astype(jnp.bfloat16))
        mixed = mixed + rounded.astype(jnp.float32)
    return (mixed.astype(jnp.bfloat16), log_weight)
```

```python
import functools

import jax
import jax.numpy as jnp
from jax import lax
from jax.experimental import pallas as pl
from jax.experimental.pallas import tpu as pltpu
from jax.sharding import PartitionSpec as P

HD = 64
WINDOW = 128
GRID_W = 64


norm_eps = 1e-06
rope_base = 10000.0
pool_reach = 8
neg_fill = -1e30


def with_halo(cells, sides, width):
    for axis, dim in sides:
        count = lax.axis_size(axis)
        ends = count - 1
        head = lax.slice_in_dim(cells, 0, width, axis=dim)
        tail = lax.slice_in_dim(cells, cells.shape[dim] - width, cells.shape[dim], axis=dim)
        cells = jnp.concatenate(
            [
                lax.ppermute(tail, axis, [(i, (i + 1) % count) for i in range(ends)]),
                cells,
                lax.ppermute(head, axis, [((i + 1) % count, i) for i in range(ends)]),
            ],
            axis=dim,
        )
    return cells


def rope_tables(positions, head_dim):
    n_freq = head_dim // 4
    freqs = rope_base ** (-jnp.arange(n_freq, dtype=jnp.float32) / n_freq)
    rows = (positions // GRID_W).astype(jnp.float32)
    columns = (positions % GRID_W).astype(jnp.float32)
    row_angle = rows[:, None] * freqs[None, :]
    col_angle = columns[:, None] * freqs[None, :]
    return (jnp.cos(row_angle), jnp.sin(row_angle), jnp.cos(col_angle), jnp.sin(col_angle))


def rotate_half(values, cosine, sine):
    middle = values.shape[-1] // 2
    first = values[..., :middle]
    second = values[..., middle:]
    return jnp.concatenate([first * cosine - second * sine, second * cosine + first * sine], -1)


def rotate_heads(values, tables, head_dim):
    rows_count = values.shape[0]
    shaped = values.astype(jnp.float32).reshape(rows_count, -1, head_dim)
    cos_r, sin_r, cos_c, sin_c = [table[:, None, :] for table in tables]
    split = head_dim // 2
    turned = jnp.concatenate(
        [
            rotate_half(shaped[..., :split], cos_r, sin_r),
            rotate_half(shaped[..., split:], cos_c, sin_c),
        ],
        -1,
    )
    return turned.reshape(rows_count, -1).astype(jnp.bfloat16)


def pool_group(extended, own, positions, half_width, seq_total):
    rows_count = own.shape[0]
    summed = jnp.zeros(own.shape, jnp.float32)
    counted = jnp.zeros((rows_count,), jnp.float32)
    for shift_by in range(-pool_reach, pool_reach):
        source = positions + shift_by
        inside = (
            (shift_by >= -half_width)
            & (shift_by < half_width)
            & (source >= 0)
            & (source < seq_total)
        )
        window_rows = extended[pool_reach + shift_by : pool_reach + shift_by + rows_count].astype(
            jnp.float32
        )
        summed = summed + jnp.where(inside[:, None], window_rows, 0.0)
        counted = counted + inside.astype(jnp.float32)
    return (summed / counted[:, None] - own.astype(jnp.float32)).astype(jnp.bfloat16)


def attend_block(queries, keys, values, sink, query_pos, key_pos, seq_total):
    scores = jnp.einsum(
        "qhgd,khd->hgqk", queries, keys, preferred_element_type=jnp.float32
    ) * HD ** (-0.5)
    valid = (
        (jnp.abs(query_pos[:, None] - key_pos[None, :]) <= WINDOW)
        & (key_pos >= 0)[None, :]
        & (key_pos < seq_total)[None, :]
    )
    scores = jnp.where(valid, scores, neg_fill)
    row_top = jnp.maximum(jnp.max(scores, -1), sink[:, :, None])
    exps = jnp.exp(scores - row_top[..., None])
    row_total = jnp.sum(exps, -1) + jnp.exp(sink[:, :, None] - row_top)
    weights = (exps / row_total[..., None]).astype(jnp.bfloat16)
    attended = jnp.einsum("hgqk,khd->qhgd", weights, values, preferred_element_type=jnp.float32)
    return (attended.astype(jnp.bfloat16), row_top + jnp.log(row_total))


def fetch_outputs(out_pool_weight, out_attn_weight):
    return (
        lax.all_gather(out_pool_weight, "sp", axis=1, tiled=True),
        lax.all_gather(out_attn_weight, "sp", axis=1, tiled=True),
    )


def local(
    tokens,
    norm_gain,
    query_weight,
    key_weight,
    value_weight,
    pool_in_weight,
    pool_mix_weight,
    sink_logit,
    out_pool_weight,
    out_attn_weight,
):
    whole = lax.all_gather(tokens, "tp", axis=1, tiled=True)
    wide = whole.astype(jnp.float32)
    normed = (
        wide * lax.rsqrt(jnp.mean(wide * wide, -1, keepdims=True) + norm_eps) * norm_gain
    ).astype(jnp.bfloat16)
    tok_rows = normed.shape[0]
    seq_total = tok_rows * lax.axis_size("sp")
    offset = lax.axis_index("sp") * tok_rows
    weights_in = (query_weight, key_weight, value_weight, pool_in_weight)
    pieces = (
        lax.all_gather(weights_in[0], "sp", axis=0, tiled=True),
        lax.all_gather(weights_in[1], "sp", axis=0, tiled=True),
        lax.all_gather(weights_in[2], "sp", axis=0, tiled=True),
        lax.all_gather(weights_in[3], "sp", axis=0, tiled=True),
    )
    sums = tuple((jnp.dot(normed, piece, preferred_element_type=jnp.float32) for piece in pieces))
    query, key, value, pool_input = [total.astype(jnp.bfloat16) for total in sums]
    positions = offset + jnp.arange(tok_rows, dtype=jnp.int32)
    tables = rope_tables(positions, HD)
    rot_query = rotate_heads(query, tables, HD)
    rot_key = rotate_heads(key, tables, HD)
    key_width = rot_key.shape[1]
    pool_ext = with_halo(pool_input, (("sp", 0),), pool_reach)
    pair_ext = with_halo(jnp.concatenate([rot_key, value], 1), (("sp", 0),), WINDOW)
    key_ext = pair_ext[:, :key_width]
    value_ext = pair_ext[:, key_width:]
    half_width = jnp.left_shift(jnp.int32(1), lax.axis_index("tp"))
    pooled = pool_group(pool_ext, pool_input, positions, half_width, seq_total)
    pool_out = jnp.dot(pooled, pool_mix_weight[0], preferred_element_type=jnp.float32).astype(
        jnp.bfloat16
    )
    heads_local = rot_query.shape[1] // HD
    kv_local = key_width // HD
    grp = heads_local // kv_local
    query_heads = rot_query.reshape(tok_rows, kv_local, grp, HD)
    key_heads = key_ext.reshape(-1, kv_local, HD)
    value_heads = value_ext.reshape(-1, kv_local, HD)
    sink = sink_logit.reshape(kv_local, grp)
    block_rows = min(tok_rows, 256)
    attended_parts = []
    log_parts = []
    for block_index in range(tok_rows // block_rows):
        start = block_index * block_rows
        query_pos = offset + start + jnp.arange(block_rows, dtype=jnp.int32)
        key_pos = offset + start - WINDOW + jnp.arange(block_rows + 2 * WINDOW, dtype=jnp.int32)
        attended_block, log_block = attend_block(
            query_heads[start : start + block_rows],
            key_heads[start : start + block_rows + 2 * WINDOW],
            value_heads[start : start + block_rows + 2 * WINDOW],
            sink,
            query_pos,
            key_pos,
            seq_total,
        )
        attended_parts.append(attended_block.reshape(block_rows, heads_local * HD))
        log_parts.append(log_block.reshape(heads_local, block_rows))
    attended = jnp.concatenate(attended_parts, 0)
    log_weight = jnp.concatenate(log_parts, 1)
    out_pool_full, out_attn_full = fetch_outputs(out_pool_weight, out_attn_weight)
    term = jnp.dot(pool_out, out_pool_full, preferred_element_type=jnp.float32)
    term = term + jnp.dot(attended, out_attn_full, preferred_element_type=jnp.float32)
    mixed = lax.psum_scatter(term.astype(jnp.bfloat16), "tp", scatter_dimension=1, tiled=True)
    return (mixed, log_weight)


NY = 2
PIECES = 2
MESH = pl.DeviceIdType.MESH


def layer_kernel(
    nz,
    ntp,
    tok_ref,
    gain_ref,
    qw_ref,
    kw_ref,
    vw_ref,
    pw_ref,
    mix_ref,
    sink_ref,
    ow_ref,
    aw_ref,
    cos_ref,
    sin_ref,
    mixed_ref,
    log_ref,
    xg,
    normed,
    wg,
    wo,
    qrot,
    ext,
    act,
    part,
    rsb,
    loc_sem,
    w_send,
    w_recv,
    x_send,
    x_recv,
    h_send,
    h_recv,
    r_send,
    r_recv,
):
    sp, tp = lax.axis_index("sp"), lax.axis_index("tp")
    nsp = nz * NY
    z, y = sp // NY, sp % NY
    rows = tok_ref.shape[0]
    width = tok_ref.shape[1]
    brow = qw_ref.shape[0]
    qn, kn, pn = qw_ref.shape[1], kw_ref.shape[1], pw_ref.shape[1]
    pool_rows = ow_ref.shape[0]
    fan = wo.shape[1]
    ocols = wo.shape[2]
    seq_total = rows * nsp
    heads, kv_local = qn // HD, kn // HD
    grp = heads // kv_local

    base = pl.multiple_of(sp * brow, brow)
    own = [
        (tok_ref, xg.at[tp]),
        (qw_ref, wg.at[pl.ds(base, brow), pl.ds(0, qn)]),
        (kw_ref, wg.at[pl.ds(base, brow), pl.ds(qn, kn)]),
        (vw_ref, wg.at[pl.ds(base, brow), pl.ds(qn + kn, kn)]),
        (pw_ref, wg.at[pl.ds(base, brow), pl.ds(qn + 2 * kn, pn)]),
        (ow_ref, wo.at[sp, pl.ds(0, pool_rows)]),
        (aw_ref, wo.at[sp, pl.ds(pool_rows, fan - pool_rows)]),
    ]
    local_copies = [pltpu.make_async_copy(a, b, loc_sem.at[i]) for i, (a, b) in enumerate(own)]
    for copy in local_copies:
        copy.start()
    ext[...] = jnp.zeros_like(ext)

    barrier = pltpu.get_barrier_semaphore()
    sp_peers = [
        (z + 1 < nz, sp + NY),
        (z >= 1, sp - NY),
        (z >= 0, z * NY + (1 - y)),
        (sp + 1 < nsp, sp + 1),
        (sp >= 1, sp - 1),
    ]
    expected = ntp - 1
    for ok, peer in sp_peers:
        expected = expected + ok.astype(jnp.int32)

        @pl.when(ok)
        def _():
            pl.semaphore_signal(barrier, inc=1, device_id={"sp": peer}, device_id_type=MESH)

    for step in range(1, ntp):
        other = lax.rem(tp + step, ntp)
        pl.semaphore_signal(barrier, inc=1, device_id={"tp": other}, device_id_type=MESH)
    for copy in local_copies:
        copy.wait()
    pl.semaphore_wait(barrier, expected)

    def weight_copy(kind, block, piece, way):
        if kind == 0:
            size = brow // PIECES
            start = pl.multiple_of(block * brow + piece * size, size)
            ref = wg.at[pl.ds(start, size)]
        else:
            size = fan // PIECES
            ref = wo.at[block, pl.ds(piece * size, size)]
        target = (sp + NY, sp - NY, z * NY + (1 - y))[way]
        return pltpu.make_async_remote_copy(
            src_ref=ref,
            dst_ref=ref,
            send_sem=w_send.at[kind, way, block, piece],
            recv_sem=w_recv.at[kind, block, piece],
            device_id={"sp": target},
            device_id_type=MESH,
        )

    onward = (z + 1 < nz, z >= 1)

    def relay(kind, d, done=False):
        def act_on(copy):
            if done:
                copy.wait_send()
            else:
                copy.start()

        for piece in range(PIECES):
            for way in range(2):
                source = (z - d, z + d)[way]
                block = source * NY + y
                if d == 0:
                    @pl.when(onward[way])
                    def _():
                        act_on(weight_copy(kind, block, piece, way))

                    if way == 1:
                        act_on(weight_copy(kind, block, piece, 2))
                else:
                    valid = (source >= 0) & (source < nz)

                    @pl.when(valid)
                    def _():
                        if not done:
                            weight_copy(kind, block, piece, 2).wait_recv()

                        @pl.when(onward[way])
                        def _():
                            act_on(weight_copy(kind, block, piece, way))

                        act_on(weight_copy(kind, block, piece, 2))

    def token_copy(step):
        other = lax.rem(tp + step, ntp)
        return pltpu.make_async_remote_copy(
            src_ref=xg.at[tp],
            dst_ref=xg.at[tp],
            send_sem=x_send.at[step],
            recv_sem=x_recv.at[tp],
            device_id={"tp": other},
            device_id_type=MESH,
        )

    def token_wait(step):
        other = lax.rem(tp + step, ntp)
        return pltpu.make_async_remote_copy(
            src_ref=xg.at[other],
            dst_ref=xg.at[other],
            send_sem=x_send.at[step],
            recv_sem=x_recv.at[other],
            device_id={"tp": other},
            device_id_type=MESH,
        )

    relay(0, 0)
    for step in range(1, ntp):
        token_copy(step).start()
    for d in range(1, nz - 1):
        relay(0, d)

    for step in range(1, ntp):
        token_wait(step).wait_recv()

    norm_rows = 64

    @pl.loop(0, rows // norm_rows)
    def _(i):
        at = pl.ds(pl.multiple_of(i * norm_rows, norm_rows), norm_rows)
        pieces = [xg[t, at, :].astype(jnp.float32) for t in range(ntp)]
        total = sum(jnp.sum(piece * piece, -1, keepdims=True) for piece in pieces)
        scale = lax.rsqrt(total / (width * ntp) + norm_eps)
        for t in range(ntp):
            cols = pl.ds(t * width, width)
            normed[at, cols] = (pieces[t] * scale * gain_ref[:, cols]).astype(jnp.bfloat16)

    for d in range(max(nz - 1, 1), nz):
        relay(0, d)
    relay(1, 0)
    for d in range(1, min(nz, 2)):
        relay(1, d)

    for source in range(nz):
        for piece in range(PIECES):
            weight_copy(0, source * NY + (1 - y), piece, 2).wait_recv()

    half = HD // 4
    lane = lax.broadcasted_iota(jnp.int32, (rows, 128), 1)
    is_first = (lane % (2 * half)) < half

    def turn(values, factor):
        wide = values.astype(jnp.bfloat16).astype(jnp.float32)
        swapped = jnp.where(
            is_first, pltpu.roll(wide, 128 - half, 1), pltpu.roll(wide, half, 1)
        )
        return ((wide * cos_ref[...] + swapped * sin_ref[...]) * factor).astype(jnp.bfloat16)

    def project(start, size):
        return jnp.dot(normed[...], wg[:, start : start + size], preferred_element_type=jnp.float32)

    mid = pl.ds(WINDOW, rows)
    for c in range(0, kn, 128):
        ext[mid, c : c + 128] = turn(project(qn + c, 128), 1.0)
    ext[mid, kn : 2 * kn] = project(qn + kn, kn).astype(jnp.bfloat16)
    ext[mid, 2 * kn : 2 * kn + pn] = project(qn + 2 * kn, pn).astype(jnp.bfloat16)
    for c in range(0, qn, 256):
        both = project(qn * 0 + c, 256)
        qrot[:, c : c + 128] = turn(both[:, :128], HD ** -0.5)
        qrot[:, c + 128 : c + 256] = turn(both[:, 128:], HD ** -0.5)

    edge = 16

    def halo_copy(way, what):
        cols = pl.ds(0, 2 * kn) if what == 0 else pl.ds(2 * kn, pn)
        count = WINDOW if what == 0 else edge
        if way == 0:
            src, dst = WINDOW + rows - count, WINDOW - count
            target = sp + 1
        else:
            src, dst = WINDOW, WINDOW + rows
            target = sp - 1
        return pltpu.make_async_remote_copy(
            src_ref=ext.at[pl.ds(src, count), cols],
            dst_ref=ext.at[pl.ds(dst, count), cols],
            send_sem=h_send.at[way, what],
            recv_sem=h_recv.at[way, what],
            device_id={"sp": target},
            device_id_type=MESH,
        )

    has_next, has_prev = sp + 1 < nsp, sp >= 1

    for way, ok in ((0, has_next), (1, has_prev)):
        @pl.when(ok)
        def _():
            halo_copy(way, 0).start()
            halo_copy(way, 1).start()

    span = 3 * WINDOW
    row_at = lax.broadcasted_iota(jnp.int32, (WINDOW, span), 0)
    key_at = lax.broadcasted_iota(jnp.int32, (WINDOW, span), 1)
    half_width = jnp.left_shift(jnp.int32(1), tp)

    def mixer_block(i):
        q_at = slice(i * WINDOW, (i + 1) * WINDOW)
        window = slice(i * WINDOW, i * WINDOW + span)
        first = sp * rows + (i - 1) * WINDOW
        inside = (key_at + first >= 0) & (key_at + first < seq_total)
        apart = key_at - row_at
        band = inside & (apart >= WINDOW - half_width) & (apart < WINDOW + half_width)
        band_f = band.astype(jnp.float32)
        counted = jnp.sum(band_f, -1, keepdims=True)
        summed = jnp.dot(
            band_f.astype(jnp.bfloat16),
            ext[window, 2 * kn : 2 * kn + pn],
            preferred_element_type=jnp.float32,
        )
        own_pool = ext[(i + 1) * WINDOW : (i + 2) * WINDOW, 2 * kn : 2 * kn + pn]
        pooled = (summed / counted - own_pool.astype(jnp.float32)).astype(jnp.bfloat16)
        act[q_at, 0:pn] = jnp.dot(
            pooled, mix_ref[...], preferred_element_type=jnp.float32
        ).astype(jnp.bfloat16)
        valid = inside & (apart >= 0) & (apart <= 2 * WINDOW)
        logs = jnp.zeros((WINDOW, 128), jnp.float32)
        lane_at = lax.broadcasted_iota(jnp.int32, (WINDOW, 128), 1)
        for kv in range(kv_local):
            keys = ext[window, kv * HD : (kv + 1) * HD]
            values = ext[window, kn + kv * HD : kn + (kv + 1) * HD]
            outs = []
            for g in range(grp):
                head = kv * grp + g
                query = qrot[q_at, head * HD : (head + 1) * HD]
                score = lax.dot_general(
                    query, keys, (((1,), (1,)), ((), ())), preferred_element_type=jnp.float32
                )
                score = jnp.where(valid, score, neg_fill)
                sink = sink_ref[head]
                top = jnp.maximum(jnp.max(score, -1, keepdims=True), sink)
                exps = jnp.exp(score - top)
                total = jnp.sum(exps, -1, keepdims=True) + jnp.exp(sink - top)
                weights = (exps * (1.0 / total)).astype(jnp.bfloat16)
                outs.append(jnp.dot(weights, values, preferred_element_type=jnp.float32))
                logs = jnp.where(lane_at == head, top + jnp.log(total), logs)
            for g in range(0, grp, 2):
                at = pn + (kv * grp + g) * HD
                act[q_at, at : at + 2 * HD] = jnp.concatenate(outs[g : g + 2], 1).astype(
                    jnp.bfloat16
                )
        log_ref[:, q_at] = logs.T[:heads, :]

    n_blocks = rows // WINDOW
    for i in range(1, n_blocks - 1):
        mixer_block(i)
        if i == 1:
            for d in range(2, min(nz, 3)):
                relay(1, d)
    for way, ok in ((0, has_prev), (1, has_next)):
        @pl.when(ok)
        def _():
            halo_copy(way, 0).wait_recv()
            halo_copy(way, 1).wait_recv()

    for i in (0, n_blocks - 1):
        mixer_block(i)
        if i == 0:
            for d in range(3, nz):
                relay(1, d)

    per_owner = nsp // ntp

    def reduce_copy(block):
        owner = block // per_owner
        slot = block % per_owner
        return pltpu.make_async_remote_copy(
            src_ref=part.at[block],
            dst_ref=rsb.at[tp, slot],
            send_sem=r_send.at[block],
            recv_sem=r_recv.at[tp, slot],
            device_id={"tp": owner},
            device_id_type=MESH,
        )

    def out_block(block):
        part[block] = jnp.dot(act[...], wo[block], preferred_element_type=jnp.float32).astype(
            jnp.bfloat16
        )

        @pl.when(block // per_owner != tp)
        def _():
            reduce_copy(block).start()

    @pl.loop(0, nz)
    def _(j):
        out_block(j * NY + y)

    @pl.loop(0, 2 * nz - 1)
    def _(k):
        d = (k + 1) // 2
        source = z + (1 - 2 * (k % 2)) * d

        @pl.when((source >= 0) & (source < nz))
        def _():
            block = source * NY + (1 - y)
            for piece in range(PIECES):
                weight_copy(1, block, piece, 2).wait_recv()
            out_block(block)

    for step in range(1, ntp):
        other = lax.rem(tp + step, ntp)
        for slot in range(per_owner):
            pltpu.make_async_remote_copy(
                src_ref=rsb.at[other, slot],
                dst_ref=rsb.at[other, slot],
                send_sem=r_send.at[slot],
                recv_sem=r_recv.at[other, slot],
                device_id={"tp": other},
                device_id_type=MESH,
            ).wait_recv()
    for slot in range(per_owner):
        total = part[tp * per_owner + slot].astype(jnp.float32)
        for step in range(1, ntp):
            total = total + rsb[lax.rem(tp + step, ntp), slot].astype(jnp.float32)
        mixed_ref[:, slot * ocols : (slot + 1) * ocols] = total.astype(jnp.bfloat16)

    for step in range(1, ntp):
        token_copy(step).wait_send()
    for kind in range(2):
        for d in range(nz):
            relay(kind, d, done=True)
    for way, ok in ((0, has_next), (1, has_prev)):
        @pl.when(ok)
        def _():
            halo_copy(way, 0).wait_send()
            halo_copy(way, 1).wait_send()

    @pl.loop(0, nsp)
    def _(block):
        @pl.when(block // per_owner != tp)
        def _():
            reduce_copy(block).wait_send()


def fused(
    nz,
    ntp,
    tokens,
    norm_gain,
    query_weight,
    key_weight,
    value_weight,
    pool_in_weight,
    pool_mix_weight,
    sink_logit,
    out_pool_weight,
    out_attn_weight,
):
    rows, width = tokens.shape
    nsp = nz * NY
    dim = width * ntp
    qn, kn, pn = query_weight.shape[1], key_weight.shape[1], pool_in_weight.shape[1]
    fan = out_pool_weight.shape[0] + out_attn_weight.shape[0]
    ocols = out_pool_weight.shape[1]
    positions = lax.axis_index("sp") * rows + jnp.arange(rows, dtype=jnp.int32)
    cos_r, sin_r, cos_c, sin_c = rope_tables(positions, HD)
    cosine = jnp.tile(jnp.concatenate([cos_r, cos_r, cos_c, cos_c], 1), (1, 128 // HD))
    sine = jnp.tile(jnp.concatenate([-sin_r, sin_r, -sin_c, sin_c], 1), (1, 128 // HD))
    hbm = pl.BlockSpec(memory_space=pl.ANY)
    vmem = pl.BlockSpec(memory_space=pltpu.VMEM)
    smem = pl.BlockSpec(memory_space=pltpu.SMEM)
    dma = pltpu.SemaphoreType.DMA
    bf16 = jnp.bfloat16
    per_owner = nsp // ntp
    return pl.pallas_call(
        functools.partial(layer_kernel, nz, ntp),
        out_shape=(
            jax.ShapeDtypeStruct((rows, width), bf16),
            jax.ShapeDtypeStruct((sink_logit.shape[0], rows), jnp.float32),
        ),
        in_specs=[hbm, vmem, hbm, hbm, hbm, hbm, vmem, smem, hbm, hbm, vmem, vmem],
        out_specs=(vmem, vmem),
        scratch_shapes=[
            pltpu.VMEM((ntp, rows, width), bf16),
            pltpu.VMEM((rows, dim), bf16),
            pltpu.VMEM((dim, qn + 2 * kn + pn), bf16),
            pltpu.VMEM((nsp, fan, ocols), bf16),
            pltpu.VMEM((rows, qn), bf16),
            pltpu.VMEM((rows + 2 * WINDOW, 2 * kn + pn), bf16),
            pltpu.VMEM((rows, fan), bf16),
            pltpu.VMEM((nsp, rows, ocols), bf16),
            pltpu.VMEM((ntp, per_owner, rows, ocols), bf16),
            dma((7,)),
            dma((2, 3, nsp, PIECES)),
            dma((2, nsp, PIECES)),
            dma((ntp,)),
            dma((ntp,)),
            dma((2, 2)),
            dma((2, 2)),
            dma((nsp,)),
            dma((ntp, per_owner)),
        ],
        compiler_params=pltpu.CompilerParams(
            collective_id=0, has_side_effects=True, vmem_limit_bytes=56 << 20
        ),
    )(
        tokens,
        norm_gain[None, :],
        query_weight,
        key_weight,
        value_weight,
        pool_in_weight,
        pool_mix_weight[0],
        sink_logit,
        out_pool_weight,
        out_attn_weight,
        cosine,
        sine,
    )


def choose(mesh):
    nsp, ntp = mesh.shape["sp"], mesh.shape["tp"]

    def body(*args):
        columns = args[8].shape[1]
        fits = nsp % NY == 0 and nsp % ntp == 0 and columns % 128 == 0
        if fits and args[0].shape[0] // WINDOW >= 2:
            return fused(nsp // NY, ntp, *args)
        return local(*args)

    return body


def solution(mesh):
    return jax.shard_map(
        choose(mesh),
        mesh=mesh,
        in_specs=(
            P("sp", "tp"),
            P(),
            P("sp", "tp"),
            P("sp", "tp"),
            P("sp", "tp"),
            P("sp", "tp"),
            P("tp", None, None),
            P("tp"),
            P("tp", "sp"),
            P("tp", "sp"),
        ),
        out_specs=(P("sp", "tp"), P("tp", "sp")),
        check_vma=False,
    )
```

```python
import functools
import math

import jax
import jax.numpy as jnp
from jax import lax
from jax.experimental import pallas as pl
from jax.experimental.pallas import tpu as pltpu
from jax.sharding import PartitionSpec as P

HD = 64
WINDOW = 128
GRID_W = 64


norm_eps = 1e-06
rope_base = 10000.0
pool_reach = 8
neg_fill = -1e30


def with_halo(cells, sides, width):
    for axis, dim in sides:
        count = lax.axis_size(axis)
        ends = count - 1
        head = lax.slice_in_dim(cells, 0, width, axis=dim)
        tail = lax.slice_in_dim(cells, cells.shape[dim] - width, cells.shape[dim], axis=dim)
        cells = jnp.concatenate(
            [
                lax.ppermute(tail, axis, [(i, (i + 1) % count) for i in range(ends)]),
                cells,
                lax.ppermute(head, axis, [((i + 1) % count, i) for i in range(ends)]),
            ],
            axis=dim,
        )
    return cells


def rope_tables(positions, head_dim):
    n_freq = head_dim // 4
    freqs = rope_base ** (-jnp.arange(n_freq, dtype=jnp.float32) / n_freq)
    rows = (positions // GRID_W).astype(jnp.float32)
    columns = (positions % GRID_W).astype(jnp.float32)
    row_angle = rows[:, None] * freqs[None, :]
    col_angle = columns[:, None] * freqs[None, :]
    return (jnp.cos(row_angle), jnp.sin(row_angle), jnp.cos(col_angle), jnp.sin(col_angle))


def rotate_half(values, cosine, sine):
    middle = values.shape[-1] // 2
    first = values[..., :middle]
    second = values[..., middle:]
    return jnp.concatenate([first * cosine - second * sine, second * cosine + first * sine], -1)


def rotate_heads(values, tables, head_dim):
    rows_count = values.shape[0]
    shaped = values.astype(jnp.float32).reshape(rows_count, -1, head_dim)
    cos_r, sin_r, cos_c, sin_c = [table[:, None, :] for table in tables]
    split = head_dim // 2
    turned = jnp.concatenate(
        [
            rotate_half(shaped[..., :split], cos_r, sin_r),
            rotate_half(shaped[..., split:], cos_c, sin_c),
        ],
        -1,
    )
    return turned.reshape(rows_count, -1).astype(jnp.bfloat16)


def pool_group(extended, own, positions, half_width, seq_total):
    rows_count = own.shape[0]
    summed = jnp.zeros(own.shape, jnp.float32)
    counted = jnp.zeros((rows_count,), jnp.float32)
    for shift_by in range(-pool_reach, pool_reach):
        source = positions + shift_by
        inside = (
            (shift_by >= -half_width)
            & (shift_by < half_width)
            & (source >= 0)
            & (source < seq_total)
        )
        window_rows = extended[pool_reach + shift_by : pool_reach + shift_by + rows_count].astype(
            jnp.float32
        )
        summed = summed + jnp.where(inside[:, None], window_rows, 0.0)
        counted = counted + inside.astype(jnp.float32)
    return (summed / counted[:, None] - own.astype(jnp.float32)).astype(jnp.bfloat16)


def attend_block(queries, keys, values, sink, query_pos, key_pos, seq_total):
    scores = jnp.einsum(
        "qhgd,khd->hgqk", queries, keys, preferred_element_type=jnp.float32
    ) * HD ** (-0.5)
    valid = (
        (jnp.abs(query_pos[:, None] - key_pos[None, :]) <= WINDOW)
        & (key_pos >= 0)[None, :]
        & (key_pos < seq_total)[None, :]
    )
    scores = jnp.where(valid, scores, neg_fill)
    row_top = jnp.maximum(jnp.max(scores, -1), sink[:, :, None])
    exps = jnp.exp(scores - row_top[..., None])
    row_total = jnp.sum(exps, -1) + jnp.exp(sink[:, :, None] - row_top)
    weights = (exps / row_total[..., None]).astype(jnp.bfloat16)
    attended = jnp.einsum("hgqk,khd->qhgd", weights, values, preferred_element_type=jnp.float32)
    return (attended.astype(jnp.bfloat16), row_top + jnp.log(row_total))


def fetch_outputs(out_pool_weight, out_attn_weight):
    return (
        lax.all_gather(out_pool_weight, "sp", axis=1, tiled=True),
        lax.all_gather(out_attn_weight, "sp", axis=1, tiled=True),
    )


def local(
    tokens,
    norm_gain,
    query_weight,
    key_weight,
    value_weight,
    pool_in_weight,
    pool_mix_weight,
    sink_logit,
    out_pool_weight,
    out_attn_weight,
):
    whole = lax.all_gather(tokens, "tp", axis=1, tiled=True)
    wide = whole.astype(jnp.float32)
    normed = (
        wide * lax.rsqrt(jnp.mean(wide * wide, -1, keepdims=True) + norm_eps) * norm_gain
    ).astype(jnp.bfloat16)
    tok_rows = normed.shape[0]
    seq_total = tok_rows * lax.axis_size("sp")
    offset = lax.axis_index("sp") * tok_rows
    weights_in = (query_weight, key_weight, value_weight, pool_in_weight)
    pieces = (
        lax.all_gather(weights_in[0], "sp", axis=0, tiled=True),
        lax.all_gather(weights_in[1], "sp", axis=0, tiled=True),
        lax.all_gather(weights_in[2], "sp", axis=0, tiled=True),
        lax.all_gather(weights_in[3], "sp", axis=0, tiled=True),
    )
    sums = tuple((jnp.dot(normed, piece, preferred_element_type=jnp.float32) for piece in pieces))
    query, key, value, pool_input = [total.astype(jnp.bfloat16) for total in sums]
    positions = offset + jnp.arange(tok_rows, dtype=jnp.int32)
    tables = rope_tables(positions, HD)
    rot_query = rotate_heads(query, tables, HD)
    rot_key = rotate_heads(key, tables, HD)
    key_width = rot_key.shape[1]
    pool_ext = with_halo(pool_input, (("sp", 0),), pool_reach)
    pair_ext = with_halo(jnp.concatenate([rot_key, value], 1), (("sp", 0),), WINDOW)
    key_ext = pair_ext[:, :key_width]
    value_ext = pair_ext[:, key_width:]
    half_width = jnp.left_shift(jnp.int32(1), lax.axis_index("tp"))
    pooled = pool_group(pool_ext, pool_input, positions, half_width, seq_total)
    pool_out = jnp.dot(pooled, pool_mix_weight[0], preferred_element_type=jnp.float32).astype(
        jnp.bfloat16
    )
    heads_local = rot_query.shape[1] // HD
    kv_local = key_width // HD
    grp = heads_local // kv_local
    query_heads = rot_query.reshape(tok_rows, kv_local, grp, HD)
    key_heads = key_ext.reshape(-1, kv_local, HD)
    value_heads = value_ext.reshape(-1, kv_local, HD)
    sink = sink_logit.reshape(kv_local, grp)
    block_rows = min(tok_rows, 256)
    attended_parts = []
    log_parts = []
    for block_index in range(tok_rows // block_rows):
        start = block_index * block_rows
        query_pos = offset + start + jnp.arange(block_rows, dtype=jnp.int32)
        key_pos = offset + start - WINDOW + jnp.arange(block_rows + 2 * WINDOW, dtype=jnp.int32)
        attended_block, log_block = attend_block(
            query_heads[start : start + block_rows],
            key_heads[start : start + block_rows + 2 * WINDOW],
            value_heads[start : start + block_rows + 2 * WINDOW],
            sink,
            query_pos,
            key_pos,
            seq_total,
        )
        attended_parts.append(attended_block.reshape(block_rows, heads_local * HD))
        log_parts.append(log_block.reshape(heads_local, block_rows))
    attended = jnp.concatenate(attended_parts, 0)
    log_weight = jnp.concatenate(log_parts, 1)
    out_pool_full, out_attn_full = fetch_outputs(out_pool_weight, out_attn_weight)
    term = jnp.dot(pool_out, out_pool_full, preferred_element_type=jnp.float32)
    term = term + jnp.dot(attended, out_attn_full, preferred_element_type=jnp.float32)
    mixed = lax.psum_scatter(term.astype(jnp.bfloat16), "tp", scatter_dimension=1, tiled=True)
    return (mixed, log_weight)


NY = 2
PIECES = 4
MESH = pl.DeviceIdType.MESH


def layer_kernel(
    nz,
    ntp,
    tok_ref,
    gain_ref,
    qw_ref,
    kw_ref,
    vw_ref,
    pw_ref,
    mix_ref,
    sink_ref,
    ow_ref,
    aw_ref,
    mixed_ref,
    log_ref,
    xg,
    normed,
    wg,
    wo,
    qrot,
    ext,
    act,
    part,
    rsb,
    cos_ref,
    sin_ref,
    pair,
    total_out,
    loc_sem,
    w_send,
    w_recv,
    x_send,
    x_recv,
    h_send,
    h_recv,
    r_send,
    r_recv,
    p_send,
    p_recv,
):
    sp, tp = lax.axis_index("sp"), lax.axis_index("tp")
    nsp = nz * NY
    z, y = sp // NY, sp % NY
    rows = tok_ref.shape[0]
    width = tok_ref.shape[1]
    brow = qw_ref.shape[0]
    qn, kn, pn = qw_ref.shape[1], kw_ref.shape[1], pw_ref.shape[1]
    pool_rows = ow_ref.shape[0]
    fan = wo.shape[1]
    ocols = wo.shape[2]
    seq_total = rows * nsp
    heads, kv_local = qn // HD, kn // HD
    grp = heads // kv_local

    base = pl.multiple_of(sp * brow, brow)
    own = [
        (tok_ref, xg.at[tp]),
        (qw_ref, wg.at[pl.ds(base, brow), pl.ds(0, qn)]),
        (kw_ref, wg.at[pl.ds(base, brow), pl.ds(qn, kn)]),
        (vw_ref, wg.at[pl.ds(base, brow), pl.ds(qn + kn, kn)]),
        (pw_ref, wg.at[pl.ds(base, brow), pl.ds(qn + 2 * kn, pn)]),
        (ow_ref, wo.at[sp, pl.ds(0, pool_rows)]),
        (aw_ref, wo.at[sp, pl.ds(pool_rows, fan - pool_rows)]),
    ]
    local_copies = [pltpu.make_async_copy(a, b, loc_sem.at[i]) for i, (a, b) in enumerate(own)]
    for copy in local_copies:
        copy.start()
    ext[...] = jnp.zeros_like(ext)

    barrier = pltpu.get_barrier_semaphore()
    sp_peers = [
        (z + 1 < nz, sp + NY),
        (z >= 1, sp - NY),
        (z >= 0, z * NY + (1 - y)),
        (sp + 1 < nsp, sp + 1),
        (sp >= 1, sp - 1),
    ]
    expected = ntp - 1
    for ok, peer in sp_peers:
        expected = expected + ok.astype(jnp.int32)

        @pl.when(ok)
        def _():
            pl.semaphore_signal(barrier, inc=1, device_id={"sp": peer}, device_id_type=MESH)

    for step in range(1, ntp):
        other = lax.rem(tp + step, ntp)
        pl.semaphore_signal(barrier, inc=1, device_id={"tp": other}, device_id_type=MESH)
    for copy in local_copies:
        copy.wait()
    pl.semaphore_wait(barrier, expected)

    def weight_copy(kind, block, piece, way):
        if kind == 0:
            size = brow // PIECES
            start = pl.multiple_of(block * brow + piece * size, size)
            ref = wg.at[pl.ds(start, size)]
        else:
            size = fan // PIECES
            ref = wo.at[block, pl.ds(piece * size, size)]
        target = (sp + NY, sp - NY, z * NY + (1 - y))[way]
        return pltpu.make_async_remote_copy(
            src_ref=ref,
            dst_ref=ref,
            send_sem=w_send.at[kind, way, block, piece],
            recv_sem=w_recv.at[kind, block, piece],
            device_id={"sp": target},
            device_id_type=MESH,
        )

    onward = (z + 1 < nz, z >= 1)

    def issue(copy, done):
        if done:
            copy.wait_send()
        else:
            copy.start()

    last = PIECES - 1

    def relay(kind, d, done=False):
        for piece in range(PIECES):
            for way in range(2):
                source = (z - d, z + d)[way]
                block = source * NY + y
                valid = (source >= 0) & (source < nz)

                @pl.when(valid)
                def _():
                    if not done:
                        weight_copy(kind, block, piece, 2).wait_recv()

                    @pl.when(onward[way])
                    def _():
                        issue(weight_copy(kind, block, piece, way), done)

                    if kind == 1 or piece != last:
                        issue(weight_copy(kind, block, piece, 2), done)

    def own_row(kind, way, done=False):
        for piece in range(PIECES):
            if way == 2:
                issue(weight_copy(kind, sp, piece, way), done)
            else:

                @pl.when(onward[way])
                def _():
                    issue(weight_copy(kind, sp, piece, way), done)

    def relay_other(d, done=False):
        if d == 0:
            block = z * NY + (1 - y)
            if not done:
                weight_copy(0, block, last, 2).wait_recv()
            for way in range(2):

                @pl.when(onward[way])
                def _():
                    issue(weight_copy(0, block, last, way), done)

        else:
            for way in range(2):
                source = (z - d, z + d)[way]

                @pl.when((source >= 0) & (source < nz))
                def _():
                    block = source * NY + (1 - y)
                    if not done:
                        weight_copy(0, block, last, 2).wait_recv()

                    @pl.when(onward[way])
                    def _():
                        issue(weight_copy(0, block, last, way), done)

    def token_copy(step):
        other = lax.rem(tp + step, ntp)
        return pltpu.make_async_remote_copy(
            src_ref=xg.at[tp],
            dst_ref=xg.at[tp],
            send_sem=x_send.at[step],
            recv_sem=x_recv.at[tp],
            device_id={"tp": other},
            device_id_type=MESH,
        )

    def token_wait(step):
        other = lax.rem(tp + step, ntp)
        return pltpu.make_async_remote_copy(
            src_ref=xg.at[other],
            dst_ref=xg.at[other],
            send_sem=x_send.at[step],
            recv_sem=x_recv.at[other],
            device_id={"tp": other},
            device_id_type=MESH,
        )

    for piece in range(PIECES):
        for way in range(2):

            @pl.when(onward[way])
            def _():
                weight_copy(0, sp, piece, way).start()

        weight_copy(0, sp, piece, 2).start()
    for step in range(1, ntp):
        token_copy(step).start()

    def out_starts(d):
        @pl.when(z == d)
        def _():
            own_row(1, 0)

        @pl.when(nz - 1 - z == d)
        def _():
            own_row(1, 1)

    half = HD // 4
    lane = lax.broadcasted_iota(jnp.int32, (rows, 128), 1)
    is_first = (lane % (2 * half)) < half
    position = sp * rows + lax.broadcasted_iota(jnp.int32, (rows, 128), 0)
    place = jnp.where((lane % HD) < 2 * half, position // GRID_W, position % GRID_W)
    freqs = jnp.exp((lane % half).astype(jnp.float32) * (-math.log(rope_base) / half))
    angle = place.astype(jnp.float32) * freqs
    cos_ref[...] = jnp.cos(angle)
    sine = jnp.sin(angle)
    sin_ref[...] = jnp.where(is_first, -sine, sine)

    for d in range(1, nz - 1):
        relay(0, d)
        relay_other(d - 1)
        out_starts(d - 1)
    own_row(1, 2)

    for step in range(1, ntp):
        token_wait(step).wait_recv()

    norm_rows = 64

    @pl.loop(0, rows // norm_rows)
    def _(i):
        at = pl.ds(pl.multiple_of(i * norm_rows, norm_rows), norm_rows)
        pieces = [xg[t, at, :].astype(jnp.float32) for t in range(ntp)]
        total = sum(jnp.sum(piece * piece, -1, keepdims=True) for piece in pieces)
        scale = lax.rsqrt(total / (width * ntp) + norm_eps)
        for t in range(ntp):
            cols = pl.ds(t * width, width)
            normed[at, cols] = (pieces[t] * scale * gain_ref[:, cols]).astype(jnp.bfloat16)

    for d in range(max(nz - 1, 1), nz):
        relay(0, d)
    for d in range(max(nz - 2, 0), nz):
        relay_other(d)
        out_starts(d)

    for source in range(nz):
        for piece in range(PIECES - 1):
            weight_copy(0, source * NY + (1 - y), piece, 2).wait_recv()

    def turn(values, factor):
        wide = values.astype(jnp.bfloat16).astype(jnp.float32)
        swapped = jnp.where(
            is_first, pltpu.roll(wide, 128 - half, 1), pltpu.roll(wide, half, 1)
        )
        return ((wide * cos_ref[...] + swapped * sin_ref[...]) * factor).astype(jnp.bfloat16)

    def project(start, size):
        return jnp.dot(normed[...], wg[:, start : start + size], preferred_element_type=jnp.float32)

    mid = pl.ds(WINDOW, rows)
    for c in range(0, kn, 128):
        ext[mid, c : c + 128] = turn(project(qn + c, 128), 1.0)
    ext[mid, kn : 2 * kn] = project(qn + kn, kn).astype(jnp.bfloat16)
    ext[mid, 2 * kn : 2 * kn + pn] = project(qn + 2 * kn, pn).astype(jnp.bfloat16)
    for c in range(0, qn, 256):
        both = project(qn * 0 + c, 256)
        qrot[:, c : c + 128] = turn(both[:, :128], HD ** -0.5)
        qrot[:, c + 128 : c + 256] = turn(both[:, 128:], HD ** -0.5)

    edge = 16

    def halo_copy(way, what):
        cols = pl.ds(0, 2 * kn) if what == 0 else pl.ds(2 * kn, pn)
        count = WINDOW if what == 0 else edge
        if way == 0:
            src, dst = WINDOW + rows - count, WINDOW - count
            target = sp + 1
        else:
            src, dst = WINDOW, WINDOW + rows
            target = sp - 1
        return pltpu.make_async_remote_copy(
            src_ref=ext.at[pl.ds(src, count), cols],
            dst_ref=ext.at[pl.ds(dst, count), cols],
            send_sem=h_send.at[way, what],
            recv_sem=h_recv.at[way, what],
            device_id={"sp": target},
            device_id_type=MESH,
        )

    has_next, has_prev = sp + 1 < nsp, sp >= 1

    for way, ok in ((0, has_next), (1, has_prev)):
        @pl.when(ok)
        def _():
            halo_copy(way, 0).start()
            halo_copy(way, 1).start()

    for d in range(1, min(nz, 2)):
        relay(1, d)

    span = 3 * WINDOW
    row_at = lax.broadcasted_iota(jnp.int32, (WINDOW, span), 0)
    key_at = lax.broadcasted_iota(jnp.int32, (WINDOW, span), 1)
    half_width = jnp.left_shift(jnp.int32(1), tp)

    def mixer_block(i):
        q_at = slice(i * WINDOW, (i + 1) * WINDOW)
        window = slice(i * WINDOW, i * WINDOW + span)
        first = sp * rows + (i - 1) * WINDOW
        inside = (key_at + first >= 0) & (key_at + first < seq_total)
        apart = key_at - row_at
        band = inside & (apart >= WINDOW - half_width) & (apart < WINDOW + half_width)
        band_f = band.astype(jnp.float32)
        counted = jnp.sum(band_f, -1, keepdims=True)
        summed = jnp.dot(
            band_f.astype(jnp.bfloat16),
            ext[window, 2 * kn : 2 * kn + pn],
            preferred_element_type=jnp.float32,
        )
        own_pool = ext[(i + 1) * WINDOW : (i + 2) * WINDOW, 2 * kn : 2 * kn + pn]
        pooled = (summed / counted - own_pool.astype(jnp.float32)).astype(jnp.bfloat16)
        act[q_at, 0:pn] = jnp.dot(
            pooled, mix_ref[0], preferred_element_type=jnp.float32
        ).astype(jnp.bfloat16)
        valid = inside & (apart >= 0) & (apart <= 2 * WINDOW)
        logs = jnp.zeros((WINDOW, 128), jnp.float32)
        lane_at = lax.broadcasted_iota(jnp.int32, (WINDOW, 128), 1)
        for kv in range(kv_local):
            keys = ext[window, kv * HD : (kv + 1) * HD]
            values = ext[window, kn + kv * HD : kn + (kv + 1) * HD]
            outs = []
            for g in range(grp):
                head = kv * grp + g
                query = qrot[q_at, head * HD : (head + 1) * HD]
                score = lax.dot_general(
                    query, keys, (((1,), (1,)), ((), ())), preferred_element_type=jnp.float32
                )
                score = jnp.where(valid, score, neg_fill)
                sink = sink_ref[head]
                top = jnp.maximum(jnp.max(score, -1, keepdims=True), sink)
                exps = jnp.exp(score - top)
                total = jnp.sum(exps, -1, keepdims=True) + jnp.exp(sink - top)
                weights = (exps * (1.0 / total)).astype(jnp.bfloat16)
                outs.append(jnp.dot(weights, values, preferred_element_type=jnp.float32))
                logs = jnp.where(lane_at == head, top + jnp.log(total), logs)
            for g in range(0, grp, 2):
                at = pn + (kv * grp + g) * HD
                act[q_at, at : at + 2 * HD] = jnp.concatenate(outs[g : g + 2], 1).astype(
                    jnp.bfloat16
                )
        log_ref[:, q_at] = logs.T[:heads, :]

    n_blocks = rows // WINDOW
    for i in range(1, n_blocks - 1):
        mixer_block(i)
    for d in range(2, min(nz, 3)):
        relay(1, d)
    for way, ok in ((0, has_prev), (1, has_next)):
        @pl.when(ok)
        def _():
            halo_copy(way, 0).wait_recv()
            halo_copy(way, 1).wait_recv()

    for i in (0, n_blocks - 1):
        mixer_block(i)

    per_owner = nsp // ntp

    mate = tp + 1 - 2 * (tp % 2)

    def on_chip(block):
        return (block // per_owner) // 2 == tp // 2

    def is_mine(block):
        return block // per_owner == tp

    def is_joined(block):
        return jnp.logical_not(on_chip(block)) & ((block // per_owner) % 2 == tp % 2)

    def is_lent(block):
        return jnp.logical_not(on_chip(block)) & ((block // per_owner) % 2 != tp % 2)

    def reduce_copy(block, source):
        slot = block % per_owner
        return pltpu.make_async_remote_copy(
            src_ref=source.at[block],
            dst_ref=rsb.at[tp, slot],
            send_sem=r_send.at[block],
            recv_sem=r_recv.at[tp, slot],
            device_id={"tp": block // per_owner},
            device_id_type=MESH,
        )

    def lend_copy(block):
        return pltpu.make_async_remote_copy(
            src_ref=part.at[block],
            dst_ref=pair.at[block],
            send_sem=p_send.at[block],
            recv_sem=p_recv.at[block],
            device_id={"tp": mate},
            device_id_type=MESH,
        )

    def out_block(block):
        part[block] = jnp.dot(act[...], wo[block], preferred_element_type=jnp.float32).astype(
            jnp.bfloat16
        )

        @pl.when(on_chip(block) & jnp.logical_not(is_mine(block)))
        def _():
            reduce_copy(block, part).start()

        @pl.when(is_lent(block))
        def _():
            lend_copy(block).start()

    def join_block(block):
        @pl.when(is_joined(block))
        def _():
            lend_copy(block).wait_recv()
            total_out[block] = (
                part[block].astype(jnp.float32) + pair[block].astype(jnp.float32)
            ).astype(jnp.bfloat16)
            reduce_copy(block, total_out).start()

    def row_steps(low, high):
        @pl.loop(2 * low, 2 * high)
        def _(k):
            d = k // 2
            source = z + (2 * (k % 2) - 1) * d

            @pl.when((source >= 0) & (source < nz) & ((d > 0) | (k % 2 == 0)))
            def _():
                out_block(source * NY + y)
                join_block(source * NY + y)

    def other_steps(low, high):
        @pl.loop(2 * low, 2 * high)
        def _(k):
            d = k // 2
            source = z + (2 * (k % 2) - 1) * d

            @pl.when((source >= 0) & (source < nz) & ((d > 0) | (k % 2 == 0)))
            def _():
                block = source * NY + (1 - y)
                for piece in range(PIECES):
                    weight_copy(1, block, piece, 2).wait_recv()
                out_block(block)
                join_block(block)

    near = min(nz, 3)
    row_steps(0, near)
    other_steps(0, min(nz, 2))
    for d in range(3, nz):
        relay(1, d)
    row_steps(near, nz)
    other_steps(min(nz, 2), nz)

    for slot in range(per_owner):
        total = part[tp * per_owner + slot].astype(jnp.float32)
        for step in range(ntp // 2):
            other = mate if step == 0 else lax.rem(tp + 2 * step, ntp)
            pltpu.make_async_remote_copy(
                src_ref=rsb.at[other, slot],
                dst_ref=rsb.at[other, slot],
                send_sem=r_send.at[slot],
                recv_sem=r_recv.at[other, slot],
                device_id={"tp": other},
                device_id_type=MESH,
            ).wait_recv()
            total = total + rsb[other, slot].astype(jnp.float32)
        mixed_ref[:, slot * ocols : (slot + 1) * ocols] = total.astype(jnp.bfloat16)

    for step in range(1, ntp):
        token_copy(step).wait_send()
    for kind in range(2):
        for way in range(3):
            own_row(kind, way, done=True)
        for d in range(1, nz):
            relay(kind, d, done=True)
    for d in range(nz):
        relay_other(d, done=True)
    for way, ok in ((0, has_next), (1, has_prev)):
        @pl.when(ok)
        def _():
            halo_copy(way, 0).wait_send()
            halo_copy(way, 1).wait_send()

    @pl.loop(0, nsp)
    def _(block):
        @pl.when((on_chip(block) & jnp.logical_not(is_mine(block))) | is_joined(block))
        def _():
            reduce_copy(block, part).wait_send()

        @pl.when(is_lent(block))
        def _():
            lend_copy(block).wait_send()


def fused(
    nz,
    ntp,
    tokens,
    norm_gain,
    query_weight,
    key_weight,
    value_weight,
    pool_in_weight,
    pool_mix_weight,
    sink_logit,
    out_pool_weight,
    out_attn_weight,
):
    rows, width = tokens.shape
    nsp = nz * NY
    dim = width * ntp
    qn, kn, pn = query_weight.shape[1], key_weight.shape[1], pool_in_weight.shape[1]
    fan = out_pool_weight.shape[0] + out_attn_weight.shape[0]
    ocols = out_pool_weight.shape[1]
    hbm = pl.BlockSpec(memory_space=pl.ANY)
    vmem = pl.BlockSpec(memory_space=pltpu.VMEM)
    smem = pl.BlockSpec(memory_space=pltpu.SMEM)
    dma = pltpu.SemaphoreType.DMA
    bf16 = jnp.bfloat16
    per_owner = nsp // ntp
    return pl.pallas_call(
        functools.partial(layer_kernel, nz, ntp),
        out_shape=(
            jax.ShapeDtypeStruct((rows, width), bf16),
            jax.ShapeDtypeStruct((sink_logit.shape[0], rows), jnp.float32),
        ),
        in_specs=[hbm, vmem, hbm, hbm, hbm, hbm, vmem, smem, hbm, hbm],
        out_specs=(vmem, vmem),
        scratch_shapes=[
            pltpu.VMEM((ntp, rows, width), bf16),
            pltpu.VMEM((rows, dim), bf16),
            pltpu.VMEM((dim, qn + 2 * kn + pn), bf16),
            pltpu.VMEM((nsp, fan, ocols), bf16),
            pltpu.VMEM((rows, qn), bf16),
            pltpu.VMEM((rows + 2 * WINDOW, 2 * kn + pn), bf16),
            pltpu.VMEM((rows, fan), bf16),
            pltpu.VMEM((nsp, rows, ocols), bf16),
            pltpu.VMEM((ntp, per_owner, rows, ocols), bf16),
            pltpu.VMEM((rows, 128), jnp.float32),
            pltpu.VMEM((rows, 128), jnp.float32),
            pltpu.VMEM((nsp, rows, ocols), bf16),
            pltpu.VMEM((nsp, rows, ocols), bf16),
            dma((7,)),
            dma((2, 3, nsp, PIECES)),
            dma((2, nsp, PIECES)),
            dma((ntp,)),
            dma((ntp,)),
            dma((2, 2)),
            dma((2, 2)),
            dma((nsp,)),
            dma((ntp, per_owner)),
            dma((nsp,)),
            dma((nsp,)),
        ],
        compiler_params=pltpu.CompilerParams(
            collective_id=0, has_side_effects=True, vmem_limit_bytes=56 << 20
        ),
    )(
        tokens,
        norm_gain[None, :],
        query_weight,
        key_weight,
        value_weight,
        pool_in_weight,
        pool_mix_weight,
        sink_logit,
        out_pool_weight,
        out_attn_weight,
    )


def choose(mesh):
    nsp, ntp = mesh.shape["sp"], mesh.shape["tp"]

    def body(*args):
        columns = args[8].shape[1]
        fits = nsp % NY == 0 and nsp % ntp == 0 and columns % 128 == 0 and ntp % 2 == 0
        if fits and args[0].shape[0] // WINDOW >= 2:
            return fused(nsp // NY, ntp, *args)
        return local(*args)

    return body


def solution(mesh):
    return jax.shard_map(
        choose(mesh),
        mesh=mesh,
        in_specs=(
            P("sp", "tp"),
            P(),
            P("sp", "tp"),
            P("sp", "tp"),
            P("sp", "tp"),
            P("sp", "tp"),
            P("tp", None, None),
            P("tp"),
            P("tp", "sp"),
            P("tp", "sp"),
        ),
        out_specs=(P("sp", "tp"), P("tp", "sp")),
        check_vma=False,
    )
```
